512 devices in a mesh: ep: 32 (over z, x), tp: 16 (over y, core).
Axes of the slice: x: 4, y: 8, z: 8, core: 2. Of those that a mesh axis runs over, the one named last changes fastest.
Arguments:
- mixer_input: bfloat16 [4096, 2048], P('ep'), may hold values from -6 to 6
- mixer_gain: float32 [2048], replicated, may hold values from 0.1 to 1.9
- query_weight: bfloat16 [2048, 2048], P(None, 'tp'), may hold values from -0.125 to 0.125
- key_weight: bfloat16 [2048, 2048], P(None, 'tp'), may hold values from -0.125 to 0.125
- value_weight: bfloat16 [2048, 2048], P(None, 'tp'), may hold values from -0.125 to 0.125
- score_offset: float32 [16], P('tp'), may hold values from -8.6 to -4
- out_weight: bfloat16 [2048, 2048], P(None, 'tp'), may hold values from -1.3203125 to 1.3203125
- expert_input: bfloat16 [4096, 2048], P('ep'), may hold values from -6 to 6
- expert_gain: float32 [2048], replicated, may hold values from 0.1 to 1.9
- route_ids: int32 [4096, 2], P('ep'), may hold values from 0 to 31, as said below
- route_weights: float32 [4096, 2], P('ep'), may hold values from 0.1 to 1
- gate_weight: bfloat16 [32, 2048, 2048], P('ep', None, 'tp'), may hold values from -0.125 to 0.125
- up_weight: bfloat16 [32, 2048, 2048], P('ep', None, 'tp'), may hold values from -0.125 to 0.125
- down_weight: bfloat16 [32, 2048, 2048], P('ep', 'tp'), may hold values from -0.1875 to 0.1875
Outputs:
- mixer_output: bfloat16 [4096, 2048], P('ep', 'tp')
- expert_output: bfloat16 [4096, 2048], P('ep', 'tp')
The draws below stay inside these ranges and needn't reach their ends.
Inputs may be any that keep to these rules, and one draw needn't show every extreme that they name: `route_ids`: each row names two different experts of one group; group g holds experts g * 8 to g * 8 + 7. Among the rows of one ep index no expert is named more than 16 times, and in every draw the experts of some group are each named exactly 16 times by the rows of every ep index.
All inputs are finite; a program needn't handle non-finite values.
Results may differ from the reference program's by a relative error of at most 0.019.
Values may be sent and summed in bfloat16 or wider, within the bound.
A program may use at most 64 MiB of HBM per device.

```python
import jax
import jax.numpy as jnp
from jax import lax

D = 2048
HEADS = 16
HD = 128
SUB = 64
FF = 2048
GROUPS = 4
TOK_A = 128
TOK_B = 128
EXPERTS = 32
CAP = 16
TOKENS_A = 4096
TOKENS_B = 4096
N_EP = 32
N_TP = 16


def draw_score_offset(key, part):
    return jax.random.uniform(key, (HEADS,), jnp.float32, -8.6, -4.0)


def draw_route_ids(key, part):
    group_count = GROUPS
    per_group = EXPERTS // GROUPS
    block_count = TOKENS_B // TOK_B
    key_busy, key_perm, key_rot = jax.random.split(jax.random.fold_in(key, 7), 3)
    busy = jax.random.randint(key_busy, (), 0, group_count)
    ranks = jax.vmap(lambda sub_key: jax.random.permutation(sub_key, TOK_B))(jax.random.split(key_perm, block_count)).astype(jnp.int32)
    half_rows = TOK_B // 2
    heavy = ranks < half_rows
    others = ranks - half_rows
    group_id = jnp.where(heavy, busy, (busy + 1 + others % (group_count - 1)) % group_count)
    within_rank = jnp.where(heavy, ranks, others // (group_count - 1))
    rotation = jax.random.randint(key_rot, (block_count, group_count), 0, per_group)
    row_rotation = jnp.take_along_axis(rotation, group_id, axis=1)
    first_pick = (within_rank % per_group + row_rotation) % per_group
    step_size = max(per_group - 1, 1)
    second_pick = (within_rank % per_group + 1 + within_rank // per_group % step_size + row_rotation) % per_group
    both = jnp.stack([group_id * per_group + first_pick, group_id * per_group + second_pick], axis=-1)
    return both.reshape(TOKENS_B, 2).astype(jnp.int32)


def with_spikes(drawn, own_key, source, target, parts, factor):
    def block_of(axis_at):
        return (jnp.arange(drawn.shape[axis_at]) // (drawn.shape[axis_at] // parts)).reshape((-1,) + (1,) * (drawn.ndim - 1 - axis_at))

    one_side = jax.random.permutation(own_key, parts)[block_of(target)]
    far = (block_of(target) + parts // 2) % parts
    return jnp.where((block_of(source) == one_side) | (block_of(source) == far), factor * drawn, drawn)


def block_scale(key, dims, shards, least, high):
    def one(axis_at, blocks):
        steps = jax.random.uniform(jax.random.fold_in(jax.random.fold_in(key, 6), axis_at), (blocks,), jnp.float32, least / len(shards), high / len(shards))
        return jnp.repeat(jnp.exp(steps), dims[axis_at] // blocks).reshape((-1,) + (1,) * (len(dims) - axis_at - 1))

    level = one(*shards[0])
    for cut in shards[1:]:
        level = level * one(*cut)
    return level


def centred(rng, shape, deviation, limit, shards=(), kind=jnp.bfloat16):
    array = jax.random.normal(rng, shape, jnp.float32) * deviation
    if len(shards) > 0:
        array = block_scale(rng, shape, shards, -0.22, 0.18) * array
    return jnp.clip(array, min=-limit, max=limit).astype(kind)


def bell_draw_with(stream_key, dims, width, limit, pieces, heavy, kind=jnp.bfloat16):
    values = width * jax.random.normal(stream_key, dims, jnp.float32)
    if pieces:
        values = values * block_scale(stream_key, dims, pieces, -0.22, 0.18)
    return jnp.clip(with_spikes(values, jax.random.fold_in(stream_key, 3), *heavy), -limit, limit).astype(kind)


def setup_inputs(seed: int = 0) -> dict:
    seeds = jax.random.split(jax.random.key(seed), 15)
    mixer_input = centred(seeds[0], (TOKENS_A, D), 1.0, 6.0, ((0, 32),))
    mixer_gain = jnp.clip(1.0 + 0.18 * jax.random.normal(seeds[1], (D,), jnp.float32), 0.1, 1.9)
    query_weight = centred(seeds[2], (D, HEADS * HD), D ** -0.5, 0.125, ((1, 16),))
    key_weight = centred(seeds[3], (D, HEADS * HD), D ** -0.5, 0.125, ((1, 16),))
    value_weight = centred(seeds[4], (D, HEADS * HD), D ** -0.5, 0.125, ((1, 16),))
    score_offset = draw_score_offset(jax.random.fold_in(seeds[14], 71), 0)
    out_weight = centred(seeds[6], (HEADS * HD, D), (10 * (HEADS * HD) ** -0.5), 1.3203125, ((1, 16),))
    expert_input = centred(seeds[7], (TOKENS_B, D), 1.0, 6.0, ((0, 32),))
    expert_gain = jnp.clip(1.0 + 0.18 * jax.random.normal(seeds[8], (D,), jnp.float32), 0.1, 1.9)
    route_ids = draw_route_ids(jax.random.fold_in(seeds[14], 71), 0)
    route_weights = jnp.clip(0.1 + 0.9 * jax.random.uniform(seeds[10], (TOKENS_B, 2), jnp.float32) ** block_scale(seeds[10], (TOKENS_B, 2), ((0, 32),), -0.2, 0.2), 0.1, 1.0)
    gate_weight = centred(seeds[11], (EXPERTS, D, FF), D ** -0.5, 0.125, ((0, 32), (2, 16)))
    up_weight = centred(seeds[12], (EXPERTS, D, FF), D ** -0.5, 0.125, ((0, 32), (2, 16)))
    down_weight = bell_draw_with(seeds[13], (EXPERTS, FF, D), FF ** -0.5, 0.1875, ((0, 32), (1, 16)), (1, 2, 16, 2.0))
    return {"mixer_input": mixer_input, "mixer_gain": mixer_gain, "query_weight": query_weight, "key_weight": key_weight, "value_weight": value_weight, "score_offset": score_offset, "out_weight": out_weight, "expert_input": expert_input, "expert_gain": expert_gain, "route_ids": route_ids, "route_weights": route_weights, "gate_weight": gate_weight, "up_weight": up_weight, "down_weight": down_weight}


epsilon = 1e-06

def rms_rows(rows_in, gain):
    values_f = rows_in.astype(jnp.float32)
    scaled = values_f * lax.rsqrt(lax.optimization_barrier(jnp.mean(values_f * values_f, axis=-1, keepdims=True)) + epsilon)
    return (scaled * gain).astype(jnp.bfloat16)

def key_block(query_blk, key_blk, value_blk, score_offset, query_start, key_start):
    head_count, query_len, head_size = query_blk.shape
    key_len = key_blk.shape[1]
    scores = jnp.einsum('hqd,hkd->hqk', query_blk.astype(jnp.float32), key_blk.astype(jnp.float32))
    scores = scores * head_size ** (-0.5) + score_offset[:, None, None]
    query_pos = query_start + jnp.arange(query_len, dtype=jnp.int32)
    key_pos = key_start + jnp.arange(key_len, dtype=jnp.int32)
    causal = (key_pos[None, :] < query_pos[:, None])[None]
    log_keep = jnp.where(causal, jax.nn.log_sigmoid(-scores), 0.0)
    suffix_ones = jnp.tril(jnp.ones((SUB, SUB), jnp.float32))
    within = jnp.einsum('hqns,sr->hqnr', log_keep.reshape(head_count, query_len, key_len // SUB, SUB), suffix_ones, precision=lax.Precision.HIGHEST)
    sub_total = within[..., 0]
    later_subs = lax.cumsum(sub_total, axis=2, reverse=True) - sub_total
    after_sum = (within + later_subs[..., None]).reshape(head_count, query_len, key_len) - log_keep
    weights = jnp.where(causal, jnp.exp(jax.nn.log_sigmoid(scores) + after_sum), 0.0).astype(jnp.bfloat16)
    block_part = jnp.einsum('hqk,hkd->hqd', weights.astype(jnp.float32), value_blk.astype(jnp.float32))
    return (block_part, lax.optimization_barrier(jnp.sum(sub_total, axis=2)))

def attention_half(mixer_input, mixer_gain, query_weight, key_weight, value_weight, score_offset, out_weight):
    normed = rms_rows(mixer_input, mixer_gain)

    def project(weight):
        made = jnp.dot(normed, weight, preferred_element_type=jnp.float32).astype(jnp.bfloat16)
        return made.reshape(TOKENS_A, HEADS, HD).transpose(1, 0, 2)
    queries = project(query_weight)
    key_all = project(key_weight)
    value_all = project(value_weight)

    def query_block(block_idx):
        query_blk = lax.dynamic_slice_in_dim(queries, block_idx * TOK_A, TOK_A, 1)

        def step(turn, carried):
            running, keep_sum = carried
            key_idx = block_idx - turn
            key_blk = lax.dynamic_slice_in_dim(key_all, key_idx * TOK_A, TOK_A, 1)
            value_blk = lax.dynamic_slice_in_dim(value_all, key_idx * TOK_A, TOK_A, 1)
            block_part, block_keep = key_block(query_blk, key_blk, value_blk, score_offset, block_idx * TOK_A, key_idx * TOK_A)
            return (running + jnp.exp(keep_sum)[..., None] * block_part, keep_sum + block_keep)
        initial = (jnp.zeros((HEADS, TOK_A, HD), jnp.float32), jnp.zeros((HEADS, TOK_A), jnp.float32))
        running, unused = lax.fori_loop(0, block_idx + 1, step, initial)
        return running.astype(jnp.bfloat16)
    blocks = lax.map(query_block, jnp.arange(N_EP, dtype=jnp.int32))
    attended = blocks.transpose(0, 2, 1, 3).reshape(TOKENS_A, HEADS * HD)
    return jnp.dot(attended, out_weight, preferred_element_type=jnp.float32).astype(jnp.bfloat16)

def expert_half(expert_input, expert_gain, route_ids, route_weights, gate_weight, up_weight, down_weight):
    normed = rms_rows(expert_input, expert_gain)
    flat_ids = route_ids.reshape(-1)
    assigns = TOKENS_B * 2
    rows_max = N_EP * CAP
    padded = jnp.concatenate([normed, jnp.zeros((1, D), jnp.bfloat16)], axis=0)

    def one_expert(gathered, expert_idx):
        chosen = jnp.nonzero(flat_ids == expert_idx, size=rows_max, fill_value=assigns)[0].astype(jnp.int32)
        row_idx = jnp.minimum(chosen // 2, TOKENS_B).astype(jnp.int32)
        rows_in = padded[row_idx]
        gate_sum = jnp.dot(rows_in, gate_weight[expert_idx], preferred_element_type=jnp.float32)
        up_sum = jnp.dot(rows_in, up_weight[expert_idx], preferred_element_type=jnp.float32)
        hidden = (jax.nn.silu(gate_sum) * up_sum).astype(jnp.bfloat16)
        partial_out = jnp.einsum('rtf,tfd->trd', hidden.reshape(rows_max, N_TP, FF // N_TP).astype(jnp.float32), down_weight[expert_idx].reshape(N_TP, FF // N_TP, D).astype(jnp.float32))
        rounded = lax.optimization_barrier(partial_out.astype(jnp.bfloat16))
        result = lax.optimization_barrier(jnp.sum(rounded.astype(jnp.float32), axis=0)).astype(jnp.bfloat16)
        return (gathered.at[chosen].set(result, mode='drop'), None)
    gathered, unused = lax.scan(one_expert, jnp.zeros((assigns, D), jnp.bfloat16), jnp.arange(EXPERTS, dtype=jnp.int32))
    mixed_rows = route_weights[:, :, None] * gathered.reshape(TOKENS_B, 2, D).astype(jnp.float32)
    return lax.optimization_barrier(jnp.sum(mixed_rows, axis=1)).astype(jnp.bfloat16)

def reference(mixer_input, mixer_gain, query_weight, key_weight, value_weight, score_offset, out_weight, expert_input, expert_gain, route_ids, route_weights, gate_weight, up_weight, down_weight):
    mixer_output = attention_half(mixer_input, mixer_gain, query_weight, key_weight, value_weight, score_offset, out_weight)
    expert_output = expert_half(expert_input, expert_gain, route_ids, route_weights, gate_weight, up_weight, down_weight)
    return (mixer_output, expert_output)
```

```python
import functools

import jax
import jax.numpy as jnp
from jax import lax
from jax.experimental import pallas as pl
from jax.experimental.pallas import tpu as pltpu
from jax.sharding import PartitionSpec as P

MESH = pl.DeviceIdType.MESH
F32 = jnp.float32
BF16 = jnp.bfloat16

NZ, NX, NY = 8, 4, 8
NEP = NZ * NX
D = 2048
HD = 128
ROWS = 128
CAP = 16
SLOTS = NEP * CAP
EPS = 1e-06
DZ_ORDER = (0, 1, 7, 2, 6, 3, 5, 4)
ORDER = "EAEAEAEAEAEAEAEAEAEAEAEAEAEA"


def dot(a, b, dims=((1,), (0,))):
    return lax.dot_general(a, b, (dims, ((), ())), preferred_element_type=F32)


def rdma(src, dst, send_sem, recv_sem, to):
    return pltpu.make_async_remote_copy(
        src_ref=src,
        dst_ref=dst,
        send_sem=send_sem,
        recv_sem=recv_sem,
        device_id=to,
        device_id_type=MESH,
    )


class Ring:
    def __init__(self, n, me, view, half, device_of, sems):
        self.n, self.me, self.view, self.half = n, me, view, half
        self.right = device_of(lax.rem(me + 1, n))
        self.left = device_of(lax.rem(me + n - 1, n))
        self.sems = sems
        self.copies = {}

    def send(self, s):
        n = self.n
        at_r = lax.rem(self.me + n - s, n)
        at_l = lax.rem(self.me + s, n)
        if s < n // 2 - 1:
            ref_r, ref_l = self.view(at_r), self.view(at_l)
        else:
            ref_r, ref_l = self.half(at_r, 0), self.half(at_l, 1)
        sr, rr, sl, rl = self.sems
        r = rdma(ref_r, ref_r, sr.at[s], rr.at[s], self.right)
        l = rdma(ref_l, ref_l, sl.at[s], rl.at[s], self.left)
        r.start()
        l.start()
        self.copies[s] = (r, l)

    def wait(self, s):
        for copy in self.copies[s]:
            copy.wait_recv()

    def drain(self):
        for pair in self.copies.values():
            for copy in pair:
                copy.wait_send()


def mega(
    off_s,
    xa_h, ga_h, wq_h, wk_h, wv_h, wo_h, xb_h, gb_h, ids_h, rw_h, wg_h, wu_h, wd_h,
    out_a, out_b,
    xa, ga, wqkv, wo, xb, gb, ids, rw, wgu, wd,
    na, q, kg, vg, wts, cum, suf, att,
    pk, pt, wth, wtl, xg, acc, po, tosend, fromp, sbr, sbl, rbr, rbl, res, ret,
    in_sem, a2a_s, a2a_r, back_s, back_r,
    kx_sem, kz_sem, vz_sem, vx_sem, at_sem, atp_s, atp_r,
    yg_sem, ygp_s, ygp_r, ex_s, ex_r, rs_sem,
):
    ep = lax.axis_index("ep")
    tp = lax.axis_index("tp")
    z, x = lax.div(ep, NX), lax.rem(ep, NX)
    y, c = lax.div(tp, 2), lax.rem(tp, 2)
    other = 1 - c

    def device(zz, xx, yy, cc):
        return (zz * NX + xx, yy * 2 + cc)

    partner = device(z, x, y, other)
    my_cols = pl.ds(pl.multiple_of(c * HD, HD), HD)

    loads = []

    def load(src, dst):
        copy = pltpu.make_async_copy(src, dst, in_sem.at[len(loads)])
        copy.start()
        loads.append(copy)
        return copy

    l_xb = load(xb_h, xb)
    l_ids = load(ids_h, ids)
    l_gb = load(gb_h, gb)
    l_xa = load(xa_h, xa)
    l_ga = load(ga_h, ga)
    l_qkv = [load(w, wqkv.at[:, pl.ds(i * HD, HD)]) for i, w in enumerate((wq_h, wk_h, wv_h))]
    l_gu = [load(w, wgu.at[:, pl.ds(i * HD, HD)]) for i, w in enumerate((wg_h, wu_h))]
    l_rw = load(rw_h, rw)
    l_wd = load(wd_h, wd)
    l_wo = load(wo_h, wo)

    barrier = pltpu.get_barrier_semaphore()

    def peer(slot, sign):
        dz = DZ_ORDER[slot // NX]
        dx = slot % NX
        if sign > 0:
            return lax.rem(z + dz, NZ), lax.rem(x + dx, NX)
        return lax.rem(z + (NZ - dz), NZ), lax.rem(x + (NX - dx), NX)

    greet = [partner]
    greet.append(device(z, x, lax.rem(y + 1, NY), c))
    greet.append(device(z, x, lax.rem(y + NY - 1, NY), c))
    for slot in range(NEP - 1, 0, -1):
        zz, xx = peer(slot, 1)
        greet.append(device(zz, xx, y, c))
    for to in greet:
        pl.semaphore_signal(barrier, inc=1, device_id=to, device_id_type=MESH)

    l_ids.wait()
    expert = lax.broadcasted_iota(jnp.int32, (NEP, ROWS), 0)
    first = (expert == ids[0:1, :]).astype(F32)
    second = (expert == ids[1:2, :]).astype(F32)
    both = first + second
    earlier = (
        lax.broadcasted_iota(jnp.int32, (ROWS, ROWS), 0)
        < lax.broadcasted_iota(jnp.int32, (ROWS, ROWS), 1)
    ).astype(BF16)
    place = dot(both.astype(BF16), earlier)
    code = jnp.where(both > 0.5, place, 100.0).astype(BF16)
    line = lax.broadcasted_iota(jnp.int32, (SLOTS, NEP), 0)
    slot_i = lax.shift_right_logical(line, 4)
    step_i = lax.shift_right_logical(slot_i, 2)
    odd = (step_i & 1) == 1
    dz_i = jnp.where(
        odd, lax.shift_right_logical(step_i + 1, 1), (NZ - lax.shift_right_logical(step_i, 1))
    )
    to_z = (z + dz_i) & (NZ - 1)
    to_x = (x + (slot_i & (NX - 1))) & (NX - 1)
    spread = (
        (to_z * NX + to_x) == lax.broadcasted_iota(jnp.int32, (SLOTS, NEP), 1)
    ).astype(BF16)
    wanted = (lax.broadcasted_iota(jnp.int32, (SLOTS, ROWS), 0) & (CAP - 1)).astype(F32)
    pick = dot(spread, code) == wanted
    pt[...] = jnp.where(pick, 1.0, 0.0).astype(BF16)

    l_xb.wait()
    l_gb.wait()
    here = pl.ds(pl.multiple_of(tp * HD, HD), HD)
    squares = []
    for r in range(0, ROWS, 16):
        v = xb[pl.ds(r, 16), :].astype(F32)
        squares.append(jnp.sum(v * v, axis=1, keepdims=True))
    mean = jnp.concatenate(squares, axis=0) * (1.0 / D)
    normed = (xb[:, here].astype(F32) * lax.rsqrt(mean + EPS) * gb[:, here]).astype(BF16)
    packed = dot(pt[...], normed).astype(BF16)
    pk[...] = packed
    xg[y, pl.ds(0, CAP), my_cols] = packed[0:CAP, :]

    pl.semaphore_wait(barrier, len(greet))

    a2a = {}
    for slot in range(1, NEP):
        zz, xx = peer(slot, 1)
        rows = pl.ds(slot * CAP, CAP)
        a2a[slot] = rdma(
            pk.at[rows, :], xg.at[y, rows, my_cols], a2a_s.at[slot], a2a_r.at[slot],
            device(zz, xx, y, c),
        )
        a2a[slot].start()

    drains = []

    def attention():
        l_xa.wait()
        l_ga.wait()
        for r in range(0, ROWS, 16):
            v = xa[pl.ds(r, 16), :].astype(F32)
            m = jnp.sum(v * v, axis=1, keepdims=True) * (1.0 / D)
            na[pl.ds(r, 16), :] = (v * lax.rsqrt(m + EPS) * ga[...]).astype(BF16)
        for copy in l_qkv:
            copy.wait()
        qkv = dot(na[...], wqkv[...])
        q[...] = qkv[:, 0:HD].astype(BF16)
        own_k = pl.ds(pl.multiple_of(ep * ROWS, ROWS), ROWS)
        own_v = pl.ds(pl.multiple_of((x * NZ + z) * ROWS, ROWS), ROWS)
        kg[own_k, :] = qkv[:, HD : 2 * HD].astype(BF16)
        vg[own_v, :] = qkv[:, 2 * HD : 3 * HD].astype(BF16)

        def k_rows(block, at, count):
            return kg.at[pl.ds(pl.multiple_of(block * ROWS + at, 16), count), :]

        def v_rows(block, at, count):
            return vg.at[pl.ds(pl.multiple_of(block * ROWS + at, 16), count), :]

        kx = Ring(
            NX, x,
            lambda p: k_rows(z * NX + p, 0, ROWS),
            lambda p, h: k_rows(z * NX + p, h * 64, 64),
            lambda p: device(z, p, y, c),
            [s.at[0] for s in kx_sem],
        )
        kz = [
            Ring(
                NZ, z,
                lambda p, i=i: k_rows(p * NX, i * 256, 256),
                lambda p, h, i=i: k_rows(p * NX, i * 256 + h * 128, 128),
                lambda p: device(p, x, y, c),
                [s.at[i] for s in kz_sem],
            )
            for i in range(2)
        ]
        vz = Ring(
            NZ, z,
            lambda p: v_rows(x * NZ + p, 0, ROWS),
            lambda p, h: v_rows(x * NZ + p, h * 64, 64),
            lambda p: device(p, x, y, c),
            [s.at[0] for s in vz_sem],
        )
        vx = [
            Ring(
                NX, x,
                lambda p, i=i: v_rows(p * NZ, i * 512, 512),
                lambda p, h, i=i: v_rows(p * NZ, i * 512 + h * 256, 256),
                lambda p: device(z, p, y, c),
                [s.at[i] for s in vx_sem],
            )
            for i in range(2)
        ]
        drains.extend([kx, *kz, vz, *vx])
        kx.send(0)
        vz.send(0)
        yield

        j = lax.broadcasted_iota(jnp.int32, (256, 256), 0) & (ROWS - 1)
        s = lax.broadcasted_iota(jnp.int32, (256, 256), 1)
        suf[...] = jnp.where((j > s) | (s >= ROWS), 1.0, 0.0).astype(BF16)
        cum[...] = jnp.zeros_like(cum)
        q_pos = ep * ROWS + lax.broadcasted_iota(jnp.int32, (ROWS, 512), 0)
        k_off = lax.broadcasted_iota(jnp.int32, (ROWS, 512), 1)

        def group(d):
            g = lax.rem(z + (NZ - d), NZ)
            keys = kg[pl.ds(pl.multiple_of(g * 512, 512), 512), :]
            zf = dot(q[...], keys, ((1,), (1,))) * (HD ** -0.5) + off_s[0]
            causal = (k_off + g * 512) < q_pos
            soft = jnp.maximum(zf, 0.0) + jnp.log(1.0 + jnp.exp(-jnp.abs(zf)))
            keep = jnp.where(causal, -soft, 0.0)
            later = cum[...]
            for b in range(NX - 1, -1, -1):
                cut = slice(b * ROWS, (b + 1) * ROWS)
                kb = keep[:, cut]
                high = kb.astype(BF16)
                low = (kb - high.astype(F32)).astype(BF16)
                sums = dot(jnp.concatenate([high, low], axis=1), suf[...])
                arg = zf[:, cut] + kb + sums[:, :ROWS] + later
                w = jnp.where(causal[:, cut], jnp.exp(arg), 0.0).astype(BF16)
                at = pl.multiple_of((b * NZ + g) * ROWS, ROWS)
                wts[:, pl.ds(at, ROWS)] = w
                later = later + sums[:, ROWS:]
            cum[...] = later

        kx.wait(0)
        kx.send(1)
        vz.wait(0)
        vz.send(1)
        yield
        kx.wait(1)
        for r in kz:
            r.send(0)
        group(0)
        yield
        vz.wait(1)
        vz.send(2)
        yield
        for s_at in range(3):
            for r in kz:
                r.wait(s_at)
                r.send(s_at + 1)
            group(s_at + 1)
            yield
            if s_at == 0:
                vz.wait(2)
                vz.send(3)
                yield
            if s_at == 1:
                vz.wait(3)
                for r in vx:
                    r.send(0)
                yield
            if s_at == 2:
                for r in vx:
                    r.wait(0)
                    r.send(1)
                yield
        for r in kz:
            r.wait(3)

        @pl.loop(4, 8)
        def _(d):
            group(d)

        yield
        for r in vx:
            r.wait(1)
        attended = dot(wts[...], vg[...]).astype(BF16)
        att[y, :, my_cols] = attended
        ring = Ring(
            NY, y,
            lambda p: att.at[p, :, my_cols],
            lambda p, h: att.at[p, pl.ds(h * 64, 64), my_cols],
            lambda p: device(z, x, p, c),
            [s.at[0] for s in at_sem],
        )
        drains.append(ring)
        across = []

        def hand_over(i):
            p = lax.rem(y + (NY - i), NY)
            ref = att.at[p, :, my_cols]
            copy = rdma(ref, ref, atp_s.at[i], atp_r.at[i], partner)
            copy.start()
            across.append(copy)

        ring.send(0)
        hand_over(0)
        yield
        for s_at in range(4):
            ring.wait(s_at)
            if s_at < 3:
                ring.send(s_at + 1)
                hand_over(s_at + 1)
                hand_over(7 - s_at)
            else:
                hand_over(4)
            yield
        for copy in across:
            copy.wait_recv()
        l_wo.wait()
        total = dot(att[0], wo[pl.ds(0, 256), :])
        for i in range(1, NY):
            total += dot(att[i], wo[pl.ds(i * 256, 256), :])
        out_a[...] = total.astype(BF16)
        for copy in across:
            copy.wait_send()
        yield

    def experts():
        yg = [
            Ring(
                NY, y,
                lambda p, h=h: xg.at[p, pl.ds(h * 256, 256), my_cols],
                lambda p, k, h=h: xg.at[p, pl.ds(h * 256 + k * 128, 128), my_cols],
                lambda p: device(z, x, p, c),
                [s.at[h] for s in yg_sem],
            )
            for h in range(2)
        ]
        drains.extend(yg)
        across = {}

        def hand_over(h, i):
            p = lax.rem(y + (NY - i), NY)
            ref = xg.at[p, pl.ds(h * 256, 256), my_cols]
            copy = rdma(ref, ref, ygp_s.at[h, i], ygp_r.at[h, i], partner)
            copy.start()
            across[h, i] = copy

        for h in range(2):
            for slot in range(h * 16, h * 16 + 16):
                if slot > 0:
                    a2a[slot].wait_recv()
            yg[h].send(0)
            hand_over(h, 0)
        yield
        for copy in l_gu:
            copy.wait()

        def multiply(i, start=False):
            for h in range(2):
                across[h, i].wait_recv()
            p = lax.rem(y + (NY - i), NY)
            part = dot(xg[p], wgu[pl.ds(pl.multiple_of(p * 256, 256), 256), :])
            if start:
                acc[...] = part
            else:
                acc[...] += part

        for s_at in range(4):
            for h in range(2):
                yg[h].wait(s_at)
                if s_at < 3:
                    yg[h].send(s_at + 1)
                    hand_over(h, s_at + 1)
                    hand_over(h, 7 - s_at)
                else:
                    hand_over(h, 4)
            if s_at == 0:
                multiply(0, True)
            else:
                multiply(s_at)
                multiply(8 - s_at)
            yield
        multiply(4)
        gate, up = acc[:, 0:HD], acc[:, HD : 2 * HD]
        hidden = (gate / (1.0 + jnp.exp(-gate)) * up).astype(BF16)
        l_wd.wait()
        trades = {}
        for i in (4, 3, 5, 2, 6, 1, 7, 0):
            p = lax.rem(y + i, NY)
            part = dot(hidden, wd[:, pl.ds(pl.multiple_of(p * 256, 256), 256)])
            lower, upper = part[:, 0:HD], part[:, HD : 2 * HD]
            po[i] = jnp.where(c == 0, lower, upper)
            tosend[i] = jnp.where(c == 0, upper, lower).astype(BF16)
            trades[i] = rdma(tosend.at[i], fromp.at[i], ex_s.at[i], ex_r.at[i], partner)
            trades[i].start()
        yield
        right = device(z, x, lax.rem(y + 1, NY), c)
        left = device(z, x, lax.rem(y + NY - 1, NY), c)
        moved = []
        last = {}
        for s_at in range(4):
            i_r, i_l = 4 - s_at, 4 + s_at
            trades[i_r].wait_recv()
            if i_l != i_r:
                trades[i_l].wait_recv()
            for h in range(2):
                base = h * 256
                if s_at == 0:
                    spans_r, spans_l = ((0, 128, False),), ((128, 128, False),)
                elif s_at == 1:
                    spans_r = ((0, 128, True), (128, 128, False))
                    spans_l = ((0, 128, False), (128, 128, True))
                else:
                    spans_r = spans_l = ((0, 256, True),)
                for way, i, spans, sent, got, to, sems in (
                    (0, i_r, spans_r, sbr, rbr, right, (rs_sem[0], rs_sem[1])),
                    (1, i_l, spans_l, sbl, rbl, left, (rs_sem[2], rs_sem[3])),
                ):
                    if s_at > 0:
                        last[way, h].wait_recv()
                    for at, count, add in spans:
                        rows = pl.ds(base + at, count)
                        value = po[i, rows, :] + fromp[i, rows, :].astype(F32)
                        if add:
                            value = value + got[s_at - 1, rows, :].astype(F32)
                        sent[s_at, rows, :] = value.astype(BF16)
                    lo = spans[0][0]
                    n = sum(span[1] for span in spans)
                    rows = pl.ds(base + lo, n)
                    copy = rdma(
                        sent.at[s_at, rows, :], got.at[s_at, rows, :],
                        sems[0].at[h, s_at], sems[1].at[h, s_at], to,
                    )
                    copy.start()
                    moved.append(copy)
                    last[way, h] = copy
            yield
        trades[0].wait_recv()
        back = {}
        for h in range(2):
            last[0, h].wait_recv()
            last[1, h].wait_recv()
            rows = pl.ds(h * 256, 256)
            value = po[0, rows, :] + fromp[0, rows, :].astype(F32)
            value = value + rbr[3, rows, :].astype(F32) + rbl[3, rows, :].astype(F32)
            res[rows, :] = value.astype(BF16)
            if h == 0:
                ret[pl.ds(0, CAP), :] = value[0:CAP, :].astype(BF16)
            for slot in range(h * 16, h * 16 + 16):
                if slot > 0:
                    zz, xx = peer(slot, -1)
                    at = pl.ds(slot * CAP, CAP)
                    back[slot] = rdma(
                        res.at[at, :], ret.at[at, :], back_s.at[slot], back_r.at[slot],
                        device(zz, xx, y, c),
                    )
                    back[slot].start()
        l_rw.wait()
        weight = first * rw[0:1, :] + second * rw[1:2, :]
        w_high = weight.astype(BF16)
        w_low = (weight - w_high.astype(F32)).astype(BF16)
        mask = pt[...].astype(F32)
        wth[...] = (dot(spread, w_high) * mask).astype(BF16)
        wtl[...] = (dot(spread, w_low) * mask).astype(BF16)
        yield
        for slot in range(1, NEP):
            back[slot].wait_recv()
        over_slots = ((0,), (0,))
        combined = dot(wth[...], ret[...], over_slots) + dot(wtl[...], ret[...], over_slots)
        out_b[...] = combined.astype(BF16)
        for copy in (*across.values(), *trades.values(), *moved, *back.values()):
            copy.wait_send()
        yield

    halves = {"E": experts(), "A": attention()}
    for name in ORDER:
        if name in halves:
            try:
                next(halves[name])
            except StopIteration:
                del halves[name]
    for rest in halves.values():
        for _ in rest:
            pass
    for copy in a2a.values():
        copy.wait_send()
    for ring in drains:
        ring.drain()


def ring_sems(count, steps):
    return [pltpu.SemaphoreType.DMA((count, steps))] * 4


def on_device(
    mixer_input, mixer_gain, query_weight, key_weight, value_weight, score_offset, out_weight,
    expert_input, expert_gain, route_ids, route_weights, gate_weight, up_weight, down_weight,
):
    hbm = pl.BlockSpec(memory_space=pl.ANY)
    vmem = pl.BlockSpec(memory_space=pltpu.VMEM)
    dma = pltpu.SemaphoreType.DMA
    out = jax.ShapeDtypeStruct((ROWS, HD), BF16)
    scratch = [
        pltpu.VMEM((ROWS, D), BF16),
        pltpu.VMEM((1, D), F32),
        pltpu.VMEM((D, 3 * HD), BF16),
        pltpu.VMEM((D, HD), BF16),
        pltpu.VMEM((ROWS, D), BF16),
        pltpu.VMEM((1, D), F32),
        pltpu.VMEM((2, ROWS), jnp.int32),
        pltpu.VMEM((2, ROWS), F32),
        pltpu.VMEM((D, 2 * HD), BF16),
        pltpu.VMEM((HD, D), BF16),
        pltpu.VMEM((ROWS, D), BF16),
        pltpu.VMEM((ROWS, HD), BF16),
        pltpu.VMEM((NEP * ROWS, HD), BF16),
        pltpu.VMEM((NEP * ROWS, HD), BF16),
        pltpu.VMEM((ROWS, NEP * ROWS), BF16),
        pltpu.VMEM((ROWS, ROWS), F32),
        pltpu.VMEM((256, 256), BF16),
        pltpu.VMEM((NY, ROWS, 2 * HD), BF16),
        pltpu.VMEM((SLOTS, HD), BF16),
        pltpu.VMEM((SLOTS, ROWS), BF16),
        pltpu.VMEM((SLOTS, ROWS), BF16),
        pltpu.VMEM((SLOTS, ROWS), BF16),
        pltpu.VMEM((NY, SLOTS, 2 * HD), BF16),
        pltpu.VMEM((SLOTS, 2 * HD), F32),
        pltpu.VMEM((NY, SLOTS, HD), F32),
        pltpu.VMEM((NY, SLOTS, HD), BF16),
        pltpu.VMEM((NY, SLOTS, HD), BF16),
        pltpu.VMEM((4, SLOTS, HD), BF16),
        pltpu.VMEM((4, SLOTS, HD), BF16),
        pltpu.VMEM((4, SLOTS, HD), BF16),
        pltpu.VMEM((4, SLOTS, HD), BF16),
        pltpu.VMEM((SLOTS, HD), BF16),
        pltpu.VMEM((SLOTS, HD), BF16),
        dma((13,)),
        dma((NEP,)), dma((NEP,)), dma((NEP,)), dma((NEP,)),
        ring_sems(1, 2), ring_sems(2, 4), ring_sems(1, 4), ring_sems(2, 2),
        ring_sems(1, 4), dma((NY,)), dma((NY,)),
        ring_sems(2, 4), dma((2, NY)), dma((2, NY)),
        dma((NY,)), dma((NY,)), ring_sems(2, 4),
    ]
    flat, tree = jax.tree.flatten(scratch)

    def body(*refs):
        fixed = 1 + 13 + 2
        mega(*refs[:fixed], *jax.tree.unflatten(tree, refs[fixed:]))

    mixed, routed = pl.pallas_call(
        body,
        out_shape=(out, out),
        in_specs=[pl.BlockSpec(memory_space=pltpu.SMEM)] + [hbm] * 13,
        out_specs=(vmem, vmem),
        scratch_shapes=flat,
        compiler_params=pltpu.CompilerParams(
            collective_id=0, has_side_effects=True, vmem_limit_bytes=60 * 1024 * 1024
        ),
        name="both_halves",
    )(
        score_offset,
        mixer_input, mixer_gain.reshape(1, D), query_weight, key_weight, value_weight, out_weight,
        expert_input, expert_gain.reshape(1, D), route_ids.T, route_weights.T,
        gate_weight.reshape(D, HD), up_weight.reshape(D, HD), down_weight.reshape(HD, D),
    )
    return mixed, routed


def solution(mesh):
    in_specs = (
        P("ep", None),
        P(),
        P(None, "tp"),
        P(None, "tp"),
        P(None, "tp"),
        P("tp"),
        P(None, "tp"),
        P("ep", None),
        P(),
        P("ep", None),
        P("ep", None),
        P("ep", None, "tp"),
        P("ep", None, "tp"),
        P("ep", "tp", None),
    )
    out_specs = (P("ep", "tp"), P("ep", "tp"))
    return jax.shard_map(
        on_device, mesh=mesh, in_specs=in_specs, out_specs=out_specs, check_vma=False
    )
```

```python
import functools

import jax
import jax.numpy as jnp
from jax import lax
from jax.experimental import pallas as pl
from jax.experimental.pallas import tpu as pltpu
from jax.sharding import PartitionSpec as P

MESH = pl.DeviceIdType.MESH
F32 = jnp.float32
BF16 = jnp.bfloat16

NZ, NX, NY = 8, 4, 8
NEP = NZ * NX
D = 2048
HD = 128
ROWS = 128
CAP = 16
SLOTS = NEP * CAP
EPS = 1e-06
DZ_ORDER = (0, 1, 7, 2, 6, 3, 5, 4)
PART = 128
PARTS = SLOTS // PART
ORDER = "".join(
    (
        "VKD0K12V30123KK01K23K0KV",
        "1K0213KK0213KK230KV1KK2W",
        "3V0K1KK2K3K0K1VO23O1023O",
        "OC",
    )
)


def dot(a, b, dims=((1,), (0,))):
    return lax.dot_general(a, b, (dims, ((), ())), preferred_element_type=F32)


def rdma(src, dst, send_sem, recv_sem, to):
    return pltpu.make_async_remote_copy(
        src_ref=src,
        dst_ref=dst,
        send_sem=send_sem,
        recv_sem=recv_sem,
        device_id=to,
        device_id_type=MESH,
    )


class Ring:
    def __init__(self, name, n, me, view, half, device_of, sems):
        self.name = name
        self.n, self.me, self.view, self.half = n, me, view, half
        self.right = device_of(lax.rem(me + 1, n))
        self.left = device_of(lax.rem(me + n - 1, n))
        self.sems = sems
        self.copies = {}

    def send(self, s):
        n = self.n
        at_r = lax.rem(self.me + n - s, n)
        at_l = lax.rem(self.me + s, n)
        if self.half is None or s < n // 2 - 1:
            ref_r, ref_l = self.view(at_r), self.view(at_l)
        else:
            ref_r, ref_l = self.half(at_r, 0), self.half(at_l, 1)
        sr, rr, sl, rl = self.sems
        r = rdma(ref_r, ref_r, sr.at[s], rr.at[s], self.right)
        l = rdma(ref_l, ref_l, sl.at[s], rl.at[s], self.left)
        r.start()
        l.start()
        self.copies[s] = (r, l)

    def wait(self, s):
        with jax.named_scope(f"{self.name}_wait#s={s}"):
            for copy in self.copies[s]:
                copy.wait_recv()

    def drain(self):
        for pair in self.copies.values():
            for copy in pair:
                copy.wait_send()


class TwoStage:
    PLAN = (
        (0, 0, 2, 2), (0, 0, 2, -2), (0, 0, 2, 1), (0, 0, 2, -1),
        (-2, 0, 1, 2), (-2, 0, 2, 1), (2, 1, 2, -2), (2, 0, 2, -1),
    )

    def __init__(self, name, me, rows, view, device_of, sems):
        self.name, self.me, self.rows = name, me, rows
        self.view, self.device_of, self.sems = view, device_of, sems
        self.copies = {}

    def place(self, offset):
        return lax.rem(self.me + 8 + offset, 8)

    def send(self, i):
        block, first, last, to = self.PLAN[i]
        half = self.rows // 2
        ref = self.view(self.place(block), first * half, (last - first) * half)
        copy = rdma(
            ref, ref, self.sems[0].at[i], self.sems[1].at[i], self.device_of(self.place(to))
        )
        copy.start()
        self.copies[i] = copy

    def start(self):
        for i in range(4):
            self.send(i)

    def wait(self, *which):
        with jax.named_scope(f"{self.name}_wait#s={which[0]}"):
            for i in which:
                self.copies[i].wait_recv()

    def drain(self):
        for copy in self.copies.values():
            copy.wait_send()


def mega(
    off_h,
    xa_h, ga_h, wq_h, wk_h, wv_h, wo_h, xb_h, gb_h, ids_h, rw_h, wg_h, wu_h, wd_h,
    out_ab,
    off, xa, ga, wqkv, wo, xb, gb, ids, rw, wgu, wd,
    na, q, kg, vg, wts, cum, suf, att,
    pk, pt, wth, wtl, xg, acc, po, tosend, fromp, sbr, sbl, rbr, rbl, res, ret,
    in_sem, a2a_s, a2a_r, back_s, back_r,
    kx_s, kx_r, kz_sem, vz_s, vz_r, vx_sem, at_s, at_r, atp_s, atp_r,
    yg_sem, ygp_s, ygp_r, ex_s, ex_r, rs_sem,
):
    ep = lax.axis_index("ep")
    tp = lax.axis_index("tp")
    z, x = lax.div(ep, NX), lax.rem(ep, NX)
    y, c = lax.div(tp, 2), lax.rem(tp, 2)
    other = 1 - c

    def device(zz, xx, yy, cc):
        return (zz * NX + xx, yy * 2 + cc)

    partner = device(z, x, y, other)
    my_cols = pl.ds(pl.multiple_of(c * HD, HD), HD)

    loads = []

    def load(src, dst):
        copy = pltpu.make_async_copy(src, dst, in_sem.at[len(loads)])
        copy.start()
        loads.append(copy)
        return copy

    l_xb = load(xb_h, xb)
    l_ids = load(ids_h, ids)
    l_gb = load(gb_h, gb)
    l_xa = load(xa_h, xa)
    l_ga = load(ga_h, ga)
    l_qkv = [load(w, wqkv.at[:, pl.ds(i * HD, HD)]) for i, w in enumerate((wq_h, wk_h, wv_h))]
    l_gu = [load(w, wgu.at[:, pl.ds(i * HD, HD)]) for i, w in enumerate((wg_h, wu_h))]
    l_rw = load(rw_h, rw)
    l_wd = load(wd_h, wd)
    l_wo = load(wo_h, wo)
    l_off = load(off_h, off)

    barrier = pltpu.get_barrier_semaphore()

    def peer(slot, sign):
        dz = DZ_ORDER[slot // NX]
        dx = slot % NX
        if sign > 0:
            return lax.rem(z + dz, NZ), lax.rem(x + dx, NX)
        return lax.rem(z + (NZ - dz), NZ), lax.rem(x + (NX - dx), NX)

    greet = [partner]
    greet.append(device(z, x, lax.rem(y + 1, NY), c))
    greet.append(device(z, x, lax.rem(y + NY - 1, NY), c))
    for slot in range(NEP - 1, 0, -1):
        zz, xx = peer(slot, 1)
        greet.append(device(zz, xx, y, c))
    for to in greet:
        pl.semaphore_signal(barrier, inc=1, device_id=to, device_id_type=MESH)

    l_ids.wait()
    expert = lax.broadcasted_iota(jnp.int32, (NEP, ROWS), 0)
    first = (expert == ids[0:1, :]).astype(F32)
    second = (expert == ids[1:2, :]).astype(F32)
    both = first + second
    earlier = (
        lax.broadcasted_iota(jnp.int32, (ROWS, ROWS), 0)
        < lax.broadcasted_iota(jnp.int32, (ROWS, ROWS), 1)
    ).astype(BF16)
    place = dot(both.astype(BF16), earlier)
    code = jnp.where(both > 0.5, place, 100.0).astype(BF16)
    line = lax.broadcasted_iota(jnp.int32, (SLOTS, NEP), 0)
    slot_i = lax.shift_right_logical(line, 4)
    step_i = lax.shift_right_logical(slot_i, 2)
    odd = (step_i & 1) == 1
    dz_i = jnp.where(
        odd, lax.shift_right_logical(step_i + 1, 1), (NZ - lax.shift_right_logical(step_i, 1))
    )
    to_z = (z + dz_i) & (NZ - 1)
    to_x = (x + (slot_i & (NX - 1))) & (NX - 1)
    spread = (
        (to_z * NX + to_x) == lax.broadcasted_iota(jnp.int32, (SLOTS, NEP), 1)
    ).astype(BF16)
    wanted = (lax.broadcasted_iota(jnp.int32, (SLOTS, ROWS), 0) & (CAP - 1)).astype(F32)
    pick = dot(spread, code) == wanted
    pt[...] = jnp.where(pick, 1.0, 0.0).astype(BF16)

    with jax.named_scope("xb_wait"):
        l_xb.wait()
        l_gb.wait()
    squares = []
    for r in range(0, ROWS, 16):
        v = xb[pl.ds(r, 16), :].astype(F32)
        squares.append(jnp.sum(v * v, axis=1, keepdims=True))
    mean = jnp.concatenate(squares, axis=0) * (1.0 / D)
    scale = lax.rsqrt(mean + EPS)
    opposite = lax.rem(y + NY // 2, NY)

    def pack(i, chip):
        cols = pl.ds(pl.multiple_of((chip * 2 + c) * HD, HD), HD)
        normed = (xb[:, cols].astype(F32) * scale * gb[:, cols]).astype(BF16)
        packed = dot(pt[...], normed).astype(BF16)
        pk[i] = packed
        xg[chip, pl.ds(0, CAP), my_cols] = packed[0:CAP, :]

    pack(0, y)
    pack(1, opposite)

    drains = []
    order_done = []

    with jax.named_scope("xa_wait"):
        l_xa.wait()
        l_ga.wait()
    for r in range(0, ROWS, 16):
        v = xa[pl.ds(r, 16), :].astype(F32)
        m = jnp.sum(v * v, axis=1, keepdims=True) * (1.0 / D)
        na[pl.ds(r, 16), :] = (v * lax.rsqrt(m + EPS) * ga[...]).astype(BF16)
    with jax.named_scope("qkv_wait"):
        for copy in l_qkv:
            copy.wait()
        l_off.wait()
    qkv = dot(na[...], wqkv[...])
    q[...] = qkv[:, 0:HD].astype(BF16)
    own_k = pl.ds(pl.multiple_of(ep * ROWS, ROWS), ROWS)
    own_v = pl.ds(pl.multiple_of((x * NZ + z) * ROWS, ROWS), ROWS)
    kg[own_k, :] = qkv[:, HD : 2 * HD].astype(BF16)
    vg[own_v, :] = qkv[:, 2 * HD : 3 * HD].astype(BF16)
    suf_j = lax.broadcasted_iota(jnp.int32, (256, 256), 0) & (ROWS - 1)
    suf_s = lax.broadcasted_iota(jnp.int32, (256, 256), 1)
    suf[...] = jnp.where((suf_j > suf_s) | (suf_s >= ROWS), 1.0, 0.0).astype(BF16)
    cum[...] = jnp.zeros_like(cum)

    with jax.named_scope("barrier_wait"):
        pl.semaphore_wait(barrier, len(greet))

    a2a = {}

    def send_rows(i, chip):
        for slot in range(1, NEP):
            zz, xx = peer(slot, 1)
            rows = pl.ds(slot * CAP, CAP)
            a2a[i, slot] = rdma(
                pk.at[i, rows, :], xg.at[chip, rows, my_cols],
                a2a_s.at[i, slot], a2a_r.at[i, slot], device(zz, xx, y, c),
            )
            a2a[i, slot].start()

    send_rows(0, y)

    def opposite_rows():
        send_rows(1, opposite)
        yield

    q_pos = ep * ROWS + lax.broadcasted_iota(jnp.int32, (ROWS, 512), 0)
    k_off = lax.broadcasted_iota(jnp.int32, (ROWS, 512), 1)

    def group(d):
        with jax.named_scope("group"):
            g = lax.rem(z + (NZ - d), NZ)
            keys = kg[pl.ds(pl.multiple_of(g * 512, 512), 512), :]
            zf = dot(q[...], keys, ((1,), (1,))) * (HD ** -0.5) + off[...]
            causal = (k_off + g * 512) < q_pos
            soft = jnp.maximum(zf, 0.0) + jnp.log(1.0 + jnp.exp(-jnp.abs(zf)))
            keep = jnp.where(causal, -soft, 0.0)
            later = cum[...]
            for b in range(NX - 1, -1, -1):
                cut = slice(b * ROWS, (b + 1) * ROWS)
                kb = keep[:, cut]
                high = kb.astype(BF16)
                low = (kb - high.astype(F32)).astype(BF16)
                sums = dot(jnp.concatenate([high, low], axis=1), suf[...])
                arg = zf[:, cut] + kb + sums[:, :ROWS] + later
                w = jnp.where(causal[:, cut], jnp.exp(arg), 0.0).astype(BF16)
                at = pl.multiple_of((b * NZ + g) * ROWS, ROWS)
                wts[:, pl.ds(at, ROWS)] = w
                later = later + sums[:, ROWS:]
            cum[...] = later

    def key_side():
        def k_rows(block, at, count):
            return kg.at[pl.ds(pl.multiple_of(block * ROWS + at, 16), count), :]

        kx = []
        for j in range(1, NX):
            ref = k_rows(ep, 0, ROWS)
            to = device(z, lax.rem(x + j, NX), y, c)
            kx.append(rdma(ref, ref, kx_s.at[j], kx_r.at[j], to))
        kz = [
            Ring(
                "kz", NZ, z,
                lambda p, j=j: k_rows(p * NX + lax.rem(x + NX - j, NX), 0, ROWS),
                lambda p, h, j=j: k_rows(p * NX + lax.rem(x + NX - j, NX), h * 64, 64),
                lambda p: device(p, x, y, c),
                [s.at[j] for s in kz_sem],
            )
            for j in range(NX)
        ]
        drains.extend(kz)
        for copy in kx:
            copy.start()
        kz[0].send(0)
        yield
        with jax.named_scope("kx_wait"):
            for j in range(1, NX):
                kx[j - 1].wait_recv()
                kz[j].send(0)
        group(0)
        yield
        for s_at in range(4):
            for r in kz:
                r.wait(s_at)
                if s_at < 3:
                    r.send(s_at + 1)
                if r is kz[-1]:
                    group(s_at + 1)
                yield
        for d in (5, 6, 7):
            group(d)
            yield
        for copy in kx:
            copy.wait_send()
        yield

    def value_side():
        def v_rows(block, at, count):
            return vg.at[pl.ds(pl.multiple_of(block * ROWS + at, 16), count), :]

        vz = TwoStage(
            "vz", z, ROWS,
            lambda p, at, count: v_rows(x * NZ + p, at, count),
            lambda p: device(p, x, y, c),
            (vz_s, vz_r),
        )
        vx = [
            Ring(
                "vx", NX, x,
                lambda p, i=i: v_rows(p * NZ, i * 256, 256),
                lambda p, h, i=i: v_rows(p * NZ, i * 256 + h * 128, 128),
                lambda p: device(z, p, y, c),
                [s.at[i] for s in vx_sem],
            )
            for i in range(4)
        ]
        drains.extend([vz, *vx])
        vz.start()
        yield
        vz.wait(0)
        vz.send(5)
        vz.send(4)
        vz.wait(1)
        vz.send(7)
        vz.send(6)
        yield
        vz.wait(2, 3, 4, 5, 6, 7)
        for r in vx:
            r.send(0)
        yield
        for r in vx:
            r.wait(0)
            r.send(1)
            if r is vx[1]:
                yield
        yield
        for r in vx:
            r.wait(1)
        yield

    def out_side():
        assert order_done.count("K") > 20 and order_done.count("V") > 5
        attended = dot(wts[...], vg[...]).astype(BF16)
        att[y, :, my_cols] = attended
        ring = TwoStage(
            "at", y, ROWS,
            lambda p, at, count: att.at[p, pl.ds(at, count), my_cols],
            lambda p: device(z, x, p, c),
            (at_s, at_r),
        )
        drains.append(ring)
        across = []

        def hand_over(i):
            p = lax.rem(y + NY + i, NY)
            ref = att.at[p, :, my_cols]
            copy = rdma(ref, ref, atp_s.at[i + 3], atp_r.at[i + 3], partner)
            copy.start()
            across.append(copy)

        ring.start()
        hand_over(0)
        yield
        ring.wait(0)
        ring.send(5)
        ring.send(4)
        ring.wait(1)
        ring.send(7)
        ring.send(6)
        hand_over(-2)
        hand_over(2)
        ring.wait(2, 3)
        hand_over(-1)
        hand_over(1)
        yield
        ring.wait(5, 7)
        hand_over(-3)
        hand_over(3)
        ring.wait(4, 6)
        hand_over(4)
        yield
        with jax.named_scope("at_pair_wait"):
            for copy in across:
                copy.wait_recv()
        l_wo.wait()
        total = dot(att[0], wo[pl.ds(0, 256), :])
        for i in range(1, NY):
            total += dot(att[i], wo[pl.ds(i * 256, 256), :])
        out_ab[0] = total.astype(BF16)
        for copy in across:
            copy.wait_send()
        yield

    back = {}

    def experts(part_at):
        base = part_at * PART
        yg = Ring(
            "yg", NY, y,
            lambda p: xg.at[p, pl.ds(base, PART), my_cols],
            None,
            lambda p: device(z, x, p, c),
            [s.at[part_at] for s in yg_sem],
        )
        drains.append(yg)
        across = {}

        def hand_over(i):
            p = lax.rem(y + (NY - i), NY)
            ref = xg.at[p, pl.ds(base, PART), my_cols]
            copy = rdma(ref, ref, ygp_s.at[part_at, i], ygp_r.at[part_at, i], partner)
            copy.start()
            across[i] = copy

        slots = range(base // CAP, (base + PART) // CAP)
        with jax.named_scope("a2a_wait"):
            for slot in slots:
                if slot > 0:
                    a2a[0, slot].wait_recv()
        yg.send(0)
        hand_over(0)
        yield
        if part_at == 0:
            for copy in l_gu:
                copy.wait()
            l_wd.wait()
        mine = pl.ds(base, PART)

        def multiply(i, start=False):
            with jax.named_scope("pair_wait"):
                across[i].wait_recv()
            p = lax.rem(y + (NY - i), NY)
            part = dot(xg[p, mine, :], wgu[pl.ds(pl.multiple_of(p * 256, 256), 256), :])
            if start:
                acc[mine, :] = part
            else:
                acc[mine, :] += part

        for s_at in range(3):
            yg.wait(s_at)
            if s_at < 2:
                yg.send(s_at + 1)
            hand_over(s_at + 1)
            hand_over(7 - s_at)
            if s_at == 1:
                with jax.named_scope("a2a_wait#far"):
                    for slot in slots:
                        if slot > 0:
                            a2a[1, slot].wait_recv()
                hand_over(4)
            if s_at == 0:
                multiply(0, True)
            else:
                multiply(s_at)
                multiply(8 - s_at)
            if s_at == 2:
                multiply(4)
            yield
        multiply(3)
        multiply(5)
        gate, up = acc[mine, 0:HD], acc[mine, HD : 2 * HD]
        hidden = (gate / (1.0 + jnp.exp(-gate)) * up).astype(BF16)
        with jax.named_scope("down"):
            part = dot(hidden, wd[...])
            for p in range(NY):
                lower = part[:, p * 256 : p * 256 + HD]
                upper = part[:, p * 256 + HD : (p + 1) * 256]
                po[p, mine, :] = jnp.where(c == 0, lower, upper)
                tosend[p, mine, :] = jnp.where(c == 0, upper, lower).astype(BF16)
        trade = rdma(
            tosend.at[:, mine, :], fromp.at[:, mine, :], ex_s.at[part_at], ex_r.at[part_at], partner
        )
        trade.start()
        yield
        right = device(z, x, lax.rem(y + 1, NY), c)
        left = device(z, x, lax.rem(y + NY - 1, NY), c)
        moved = []
        last = {}
        half = PART // 2
        for s_at in range(4):
            i_r, i_l = 4 - s_at, 4 + s_at
            if s_at == 0:
                with jax.named_scope("trade_wait"):
                    trade.wait_recv()
            if s_at == 0:
                spans_r, spans_l = ((0, half, False),), ((half, half, False),)
            elif s_at == 1:
                spans_r = ((0, half, True), (half, half, False))
                spans_l = ((0, half, False), (half, half, True))
            else:
                spans_r = spans_l = ((0, PART, True),)
            for way, i, spans, sent, got, to, sems in (
                (0, i_r, spans_r, sbr, rbr, right, (rs_sem[0], rs_sem[1])),
                (1, i_l, spans_l, sbl, rbl, left, (rs_sem[2], rs_sem[3])),
            ):
                if s_at > 0:
                    with jax.named_scope(f"rs_wait#s={s_at}"):
                        last[way].wait_recv()
                p = lax.rem(y + i, NY)
                for at, count, add in spans:
                    rows = pl.ds(base + at, count)
                    value = po[p, rows, :] + fromp[p, rows, :].astype(F32)
                    if add:
                        value = value + got[s_at - 1, rows, :].astype(F32)
                    sent[s_at, rows, :] = value.astype(BF16)
                lo = spans[0][0]
                n = sum(span[1] for span in spans)
                rows = pl.ds(base + lo, n)
                copy = rdma(
                    sent.at[s_at, rows, :], got.at[s_at, rows, :],
                    sems[0].at[part_at, s_at], sems[1].at[part_at, s_at], to,
                )
                copy.start()
                moved.append(copy)
                last[way] = copy
            yield
        with jax.named_scope("rs_wait#s=4"):
            last[0].wait_recv()
            last[1].wait_recv()
        value = po[y, mine, :] + fromp[y, mine, :].astype(F32)
        value = value + rbr[3, mine, :].astype(F32) + rbl[3, mine, :].astype(F32)
        res[mine, :] = value.astype(BF16)
        if part_at == 0:
            ret[pl.ds(0, CAP), :] = value[0:CAP, :].astype(BF16)
        for slot in slots:
            if slot > 0:
                zz, xx = peer(slot, -1)
                at = pl.ds(slot * CAP, CAP)
                back[slot] = rdma(
                    res.at[at, :], ret.at[at, :], back_s.at[slot], back_r.at[slot],
                    device(zz, xx, y, c),
                )
                back[slot].start()
        yield
        for copy in (*across.values(), trade, *moved):
            copy.wait_send()
        yield

    def route_weights():
        l_rw.wait()
        weight = first * rw[0:1, :] + second * rw[1:2, :]
        w_high = weight.astype(BF16)
        w_low = (weight - w_high.astype(F32)).astype(BF16)
        mask = pt[...].astype(F32)
        wth[...] = (dot(spread, w_high) * mask).astype(BF16)
        wtl[...] = (dot(spread, w_low) * mask).astype(BF16)
        yield

    def combine():
        with jax.named_scope("back_wait"):
            for slot in range(1, NEP):
                back[slot].wait_recv()
        over_slots = ((0,), (0,))
        combined = dot(wth[...], ret[...], over_slots) + dot(wtl[...], ret[...], over_slots)
        out_ab[1] = combined.astype(BF16)
        for copy in back.values():
            copy.wait_send()
        yield

    tasks = {str(i): experts(i) for i in range(PARTS)}
    tasks.update({"K": key_side(), "V": value_side(), "O": out_side(), "D": opposite_rows(), "W": route_weights(), "C": combine()})
    for name in ORDER:
        order_done.append(name)
        if name in tasks:
            try:
                with jax.named_scope(name):
                    next(tasks[name])
            except StopIteration:
                del tasks[name]
    for rest in tasks.values():
        with jax.named_scope("rest"):
            for _ in rest:
                pass
    with jax.named_scope("drain"):
        for copy in a2a.values():
            copy.wait_send()
        for ring in drains:
            ring.drain()


def ring_sems(count, steps):
    return [pltpu.SemaphoreType.DMA((count, steps))] * 4


def on_device(
    mixer_input, mixer_gain, query_weight, key_weight, value_weight, score_offset, out_weight,
    expert_input, expert_gain, route_ids, route_weights, gate_weight, up_weight, down_weight,
):
    hbm = pl.BlockSpec(memory_space=pl.ANY)
    vmem = pl.BlockSpec(memory_space=pltpu.VMEM)
    dma = pltpu.SemaphoreType.DMA
    out = pltpu.VMEM((2, ROWS, HD), BF16)
    scratch = [
        pltpu.VMEM((1, 1), F32),
        pltpu.VMEM((ROWS, D), BF16),
        pltpu.VMEM((1, D), F32),
        pltpu.VMEM((D, 3 * HD), BF16),
        pltpu.VMEM((D, HD), BF16),
        pltpu.VMEM((ROWS, D), BF16),
        pltpu.VMEM((1, D), F32),
        pltpu.VMEM((2, ROWS), jnp.int32),
        pltpu.VMEM((2, ROWS), F32),
        pltpu.VMEM((D, 2 * HD), BF16),
        pltpu.VMEM((HD, D), BF16),
        pltpu.VMEM((ROWS, D), BF16),
        pltpu.VMEM((ROWS, HD), BF16),
        pltpu.VMEM((NEP * ROWS, HD), BF16),
        pltpu.VMEM((NEP * ROWS, HD), BF16),
        pltpu.VMEM((ROWS, NEP * ROWS), BF16),
        pltpu.VMEM((ROWS, ROWS), F32),
        pltpu.VMEM((256, 256), BF16),
        pltpu.VMEM((NY, ROWS, 2 * HD), BF16),
        pltpu.VMEM((2, SLOTS, HD), BF16),
        pltpu.VMEM((SLOTS, ROWS), BF16),
        pltpu.VMEM((SLOTS, ROWS), BF16),
        pltpu.VMEM((SLOTS, ROWS), BF16),
        pltpu.VMEM((NY, SLOTS, 2 * HD), BF16),
        pltpu.VMEM((SLOTS, 2 * HD), F32),
        pltpu.VMEM((NY, SLOTS, HD), F32),
        pltpu.VMEM((NY, SLOTS, HD), BF16),
        pltpu.VMEM((NY, SLOTS, HD), BF16),
        pltpu.VMEM((4, SLOTS, HD), BF16),
        pltpu.VMEM((4, SLOTS, HD), BF16),
        pltpu.VMEM((4, SLOTS, HD), BF16),
        pltpu.VMEM((4, SLOTS, HD), BF16),
        pltpu.VMEM((SLOTS, HD), BF16),
        pltpu.VMEM((SLOTS, HD), BF16),
    ]
    semaphores = [
        dma((14,)),
        dma((2, NEP)), dma((2, NEP)), dma((NEP,)), dma((NEP,)),
        dma((NX,)), dma((NX,)), ring_sems(4, 4), dma((8,)), dma((8,)), ring_sems(4, 2),
        dma((8,)), dma((8,)), dma((NY,)), dma((NY,)),
        ring_sems(PARTS, 4), dma((PARTS, NY)), dma((PARTS, NY)),
        dma((PARTS,)), dma((PARTS,)), ring_sems(PARTS, 4),
    ]
    flat, tree = jax.tree.flatten(semaphores)

    def body(*refs):
        def scoped(*sems):
            mega(*refs, *jax.tree.unflatten(tree, sems))

        pl.run_scoped(scoped, *flat)

    both = pl.pallas_call(
        body,
        out_shape=out,
        in_specs=[hbm] * 14,
        out_specs=vmem,
        scratch_shapes=scratch,
        compiler_params=pltpu.CompilerParams(
            collective_id=0, has_side_effects=True, vmem_limit_bytes=60 * 1024 * 1024
        ),
        name="both_halves",
    )(
        score_offset.reshape(1, 1),
        mixer_input, mixer_gain.reshape(1, D), query_weight, key_weight, value_weight, out_weight,
        expert_input, expert_gain.reshape(1, D), route_ids.T, route_weights.T,
        gate_weight.reshape(D, HD), up_weight.reshape(D, HD), down_weight.reshape(HD, D),
    )
    return both[0], both[1]


def solution(mesh):
    in_specs = (
        P("ep", None),
        P(),
        P(None, "tp"),
        P(None, "tp"),
        P(None, "tp"),
        P("tp"),
        P(None, "tp"),
        P("ep", None),
        P(),
        P("ep", None),
        P("ep", None),
        P("ep", None, "tp"),
        P("ep", None, "tp"),
        P("ep", "tp", None),
    )
    out_specs = (P("ep", "tp"), P("ep", "tp"))
    return jax.shard_map(
        on_device, mesh=mesh, in_specs=in_specs, out_specs=out_specs, check_vma=False
    )
```

```python
import functools

import jax
import jax.numpy as jnp
from jax import lax
from jax.experimental import pallas as pl
from jax.experimental.pallas import tpu as pltpu
from jax.sharding import PartitionSpec as P

MESH = pl.DeviceIdType.MESH
F32 = jnp.float32
BF16 = jnp.bfloat16

NZ, NX, NY = 8, 4, 8
NEP = NZ * NX
D = 2048
HD = 128
ROWS = 128
CAP = 16
SLOTS = NEP * CAP
EPS = 1e-06
DZ_ORDER = (0, 1, 7, 2, 6, 3, 5, 4)
PART = 128
PARTS = SLOTS // PART
ORDER = "".join(
    (
        "VWDK012VK301G2K301KV2K3K",
        "0GK10K23K1K03VK123GKK0VK",
        "2G1G3KG0KGK2KG1VO032FO13",
        "2FOOXC",
    )
)


def dot(a, b, dims=((1,), (0,))):
    return lax.dot_general(a, b, (dims, ((), ())), preferred_element_type=F32)


def rdma(src, dst, send_sem, recv_sem, to):
    return pltpu.make_async_remote_copy(
        src_ref=src,
        dst_ref=dst,
        send_sem=send_sem,
        recv_sem=recv_sem,
        device_id=to,
        device_id_type=MESH,
    )


class Ring:
    def __init__(self, name, n, me, view, half, device_of, sems):
        self.name = name
        self.n, self.me, self.view, self.half = n, me, view, half
        self.right = device_of(lax.rem(me + 1, n))
        self.left = device_of(lax.rem(me + n - 1, n))
        self.sems = sems
        self.copies = {}

    def send(self, s):
        n = self.n
        at_r = lax.rem(self.me + n - s, n)
        at_l = lax.rem(self.me + s, n)
        if self.half is None or s < n // 2 - 1:
            ref_r, ref_l = self.view(at_r), self.view(at_l)
        else:
            ref_r, ref_l = self.half(at_r, 0), self.half(at_l, 1)
        sr, rr, sl, rl = self.sems
        r = rdma(ref_r, ref_r, sr.at[s], rr.at[s], self.right)
        l = rdma(ref_l, ref_l, sl.at[s], rl.at[s], self.left)
        r.start()
        l.start()
        self.copies[s] = (r, l)

    def wait(self, s):
        with jax.named_scope(f"{self.name}_wait#s={s}"):
            for copy in self.copies[s]:
                copy.wait_recv()

    def drain(self):
        for pair in self.copies.values():
            for copy in pair:
                copy.wait_send()


class TwoStage:
    PLAN = (
        (0, 0, 2, 2), (0, 0, 2, -2), (0, 0, 2, 1), (0, 0, 2, -1),
        (-2, 0, 1, 2), (-2, 0, 2, 1), (2, 1, 2, -2), (2, 0, 2, -1),
    )

    def __init__(self, name, me, rows, view, device_of, sems):
        self.name, self.me, self.rows = name, me, rows
        self.view, self.device_of, self.sems = view, device_of, sems
        self.copies = {}

    def place(self, offset):
        return lax.rem(self.me + 8 + offset, 8)

    def send(self, i):
        block, first, last, to = self.PLAN[i]
        half = self.rows // 2
        ref = self.view(self.place(block), first * half, (last - first) * half)
        copy = rdma(
            ref, ref, self.sems[0].at[i], self.sems[1].at[i], self.device_of(self.place(to))
        )
        copy.start()
        self.copies[i] = copy

    def start(self):
        for i in range(4):
            self.send(i)

    def wait(self, *which):
        with jax.named_scope(f"{self.name}_wait#s={which[0]}"):
            for i in which:
                self.copies[i].wait_recv()

    def drain(self):
        for copy in self.copies.values():
            copy.wait_send()


def mega(
    off_h,
    xa_h, ga_h, wq_h, wk_h, wv_h, wo_h, xb_h, gb_h, ids_h, rw_h, wg_h, wu_h, wd_h,
    out_ab,
    off, xa, ga, wqkv, wo, xb, gb, ids, rw, wgu, wd,
    na, q, kg, vg, wts, cum, suf, att,
    pk, pt, wth, wtl, xg, acc, po, tosend, fromp, sbr, sbl, rbr, rbl, res, ret, far, farin,
    in_sem, a2a_s, a2a_r, back_s, back_r, far_s, far_r,
    kx_s, kx_r, kz_sem, vz_s, vz_r, vx_sem, at_s, at_r, atp_s, atp_r,
    yg_sem, ygp_s, ygp_r, ex_s, ex_r, rs_sem,
):
    ep = lax.axis_index("ep")
    tp = lax.axis_index("tp")
    z, x = lax.div(ep, NX), lax.rem(ep, NX)
    y, c = lax.div(tp, 2), lax.rem(tp, 2)
    other = 1 - c

    def device(zz, xx, yy, cc):
        return (zz * NX + xx, yy * 2 + cc)

    partner = device(z, x, y, other)
    my_cols = pl.ds(pl.multiple_of(c * HD, HD), HD)

    barrier = pltpu.get_barrier_semaphore()

    def peer(slot, sign):
        dz = DZ_ORDER[slot // NX]
        dx = slot % NX
        if sign > 0:
            return lax.rem(z + dz, NZ), lax.rem(x + dx, NX)
        return lax.rem(z + (NZ - dz), NZ), lax.rem(x + (NX - dx), NX)

    greet = [partner]
    greet.append(device(z, x, lax.rem(y + 1, NY), c))
    greet.append(device(z, x, lax.rem(y + NY - 1, NY), c))
    for slot in range(NEP - 1, 0, -1):
        zz, xx = peer(slot, 1)
        greet.append(device(zz, xx, y, c))
    for to in greet:
        pl.semaphore_signal(barrier, inc=1, device_id=to, device_id_type=MESH)

    loads = []

    def load(src, dst):
        copy = pltpu.make_async_copy(src, dst, in_sem.at[len(loads)])
        copy.start()
        loads.append(copy)
        return copy

    l_xb = load(xb_h, xb)
    l_ids = load(ids_h, ids)
    l_gb = load(gb_h, gb)
    l_xa = load(xa_h, xa)
    l_ga = load(ga_h, ga)
    l_qkv = [load(w, wqkv.at[:, pl.ds(i * HD, HD)]) for i, w in enumerate((wq_h, wk_h, wv_h))]
    l_gu = [load(w, wgu.at[:, pl.ds(i * HD, HD)]) for i, w in enumerate((wg_h, wu_h))]
    l_rw = load(rw_h, rw)
    l_wd = load(wd_h, wd)
    l_wo = load(wo_h, wo)
    l_off = load(off_h, off)

    l_ids.wait()
    expert = lax.broadcasted_iota(jnp.int32, (NEP, ROWS), 0)
    first = (expert == ids[0:1, :]).astype(F32)
    second = (expert == ids[1:2, :]).astype(F32)
    both = first + second
    earlier = (
        lax.broadcasted_iota(jnp.int32, (ROWS, ROWS), 0)
        < lax.broadcasted_iota(jnp.int32, (ROWS, ROWS), 1)
    ).astype(BF16)
    place = dot(both.astype(BF16), earlier)
    code = jnp.where(both > 0.5, place, 100.0).astype(BF16)
    line = lax.broadcasted_iota(jnp.int32, (SLOTS, NEP), 0)
    slot_i = lax.shift_right_logical(line, 4)
    step_i = lax.shift_right_logical(slot_i, 2)
    odd = (step_i & 1) == 1
    dz_i = jnp.where(
        odd, lax.shift_right_logical(step_i + 1, 1), (NZ - lax.shift_right_logical(step_i, 1))
    )
    to_z = (z + dz_i) & (NZ - 1)
    to_x = (x + (slot_i & (NX - 1))) & (NX - 1)
    spread = (
        (to_z * NX + to_x) == lax.broadcasted_iota(jnp.int32, (SLOTS, NEP), 1)
    ).astype(BF16)
    wanted = (lax.broadcasted_iota(jnp.int32, (SLOTS, ROWS), 0) & (CAP - 1)).astype(F32)
    pick = dot(spread, code) == wanted
    pt[...] = jnp.where(pick, 1.0, 0.0).astype(BF16)

    with jax.named_scope("xb_wait"):
        l_xb.wait()
        l_gb.wait()
    squares = []
    for r in range(0, ROWS, 16):
        v = xb[pl.ds(r, 16), :].astype(F32)
        squares.append(jnp.sum(v * v, axis=1, keepdims=True))
    mean = jnp.concatenate(squares, axis=0) * (1.0 / D)
    scale = lax.rsqrt(mean + EPS)
    opposite = lax.rem(y + NY // 2, NY)

    def pack(i, chip):
        cols = pl.ds(pl.multiple_of((chip * 2 + c) * HD, HD), HD)
        normed = (xb[:, cols].astype(F32) * scale * gb[:, cols]).astype(BF16)
        packed = dot(pt[...], normed).astype(BF16)
        pk[i] = packed
        xg[chip, pl.ds(0, CAP), my_cols] = packed[0:CAP, :]

    pack(0, y)
    pack(1, opposite)

    drains = []
    order_done = []

    with jax.named_scope("xa_wait"):
        l_xa.wait()
        l_ga.wait()
    for r in range(0, ROWS, 16):
        v = xa[pl.ds(r, 16), :].astype(F32)
        m = jnp.sum(v * v, axis=1, keepdims=True) * (1.0 / D)
        na[pl.ds(r, 16), :] = (v * lax.rsqrt(m + EPS) * ga[...]).astype(BF16)
    with jax.named_scope("qkv_wait"):
        for copy in l_qkv:
            copy.wait()
        l_off.wait()
    qkv = dot(na[...], wqkv[...])
    q[...] = qkv[:, 0:HD].astype(BF16)
    own_k = pl.ds(pl.multiple_of(ep * ROWS, ROWS), ROWS)
    own_v = pl.ds(pl.multiple_of(x * ROWS, ROWS), ROWS)
    kg[own_k, :] = qkv[:, HD : 2 * HD].astype(BF16)
    vg[z, own_v, :] = qkv[:, 2 * HD : 3 * HD].astype(BF16)
    suf_j = lax.broadcasted_iota(jnp.int32, (256, 256), 0) & (ROWS - 1)
    suf_s = lax.broadcasted_iota(jnp.int32, (256, 256), 1)
    suf[...] = jnp.where((suf_j > suf_s) | (suf_s >= ROWS), 1.0, 0.0).astype(BF16)

    with jax.named_scope("barrier_wait"):
        pl.semaphore_wait(barrier, len(greet))

    a2a = {}

    def send_rows(i, chip):
        for slot in range(1, NEP):
            zz, xx = peer(slot, 1)
            rows = pl.ds(slot * CAP, CAP)
            a2a[i, slot] = rdma(
                pk.at[i, rows, :], xg.at[chip, rows, my_cols],
                a2a_s.at[i, slot], a2a_r.at[i, slot], device(zz, xx, y, c),
            )
            a2a[i, slot].start()

    send_rows(0, y)

    def opposite_rows():
        send_rows(1, opposite)
        yield

    q_pos = ep * ROWS + lax.broadcasted_iota(jnp.int32, (ROWS, 512), 0)
    k_off = lax.broadcasted_iota(jnp.int32, (ROWS, 512), 1)

    def group(d):
        with jax.named_scope("group"):
            g = lax.rem(z + (NZ - d), NZ)
            keys = kg[pl.ds(pl.multiple_of(g * 512, 512), 512), :]
            zf = dot(q[...], keys, ((1,), (1,))) * (HD ** -0.5) + off[...]
            causal = (k_off + g * 512) < q_pos
            soft = jnp.maximum(zf, 0.0) + jnp.log(1.0 + jnp.exp(-jnp.abs(zf)))
            keep = jnp.where(causal, -soft, 0.0)
            later = None
            for b in range(NX - 1, -1, -1):
                cut = slice(b * ROWS, (b + 1) * ROWS)
                kb = keep[:, cut]
                high = kb.astype(BF16)
                low = (kb - high.astype(F32)).astype(BF16)
                sums = dot(jnp.concatenate([high, low], axis=1), suf[...])
                arg = zf[:, cut] + kb + sums[:, :ROWS]
                if later is not None:
                    arg = arg + later
                w = jnp.where(causal[:, cut], jnp.exp(arg), 0.0).astype(BF16)
                wts[d, :, cut] = w
                later = sums[:, ROWS:] if later is None else later + sums[:, ROWS:]
            cum[d] = later

    def groups():
        for d, needed in ((0, 2), (1, 6), (7, 6), (2, 10), (6, 10), (3, 14), (5, 14), (4, 18)):
            assert order_done.count("K") >= needed
            group(d)
            yield

    def key_side():
        def k_rows(block, at, count):
            return kg.at[pl.ds(pl.multiple_of(block * ROWS + at, 16), count), :]

        kx = []
        for j in range(1, NX):
            ref = k_rows(ep, 0, ROWS)
            to = device(z, lax.rem(x + j, NX), y, c)
            kx.append(rdma(ref, ref, kx_s.at[j], kx_r.at[j], to))
        kz = [
            Ring(
                "kz", NZ, z,
                lambda p, j=j: k_rows(p * NX + lax.rem(x + NX - j, NX), 0, ROWS),
                lambda p, h, j=j: k_rows(p * NX + lax.rem(x + NX - j, NX), h * 64, 64),
                lambda p: device(p, x, y, c),
                [s.at[j] for s in kz_sem],
            )
            for j in range(NX)
        ]
        drains.extend(kz)
        for copy in kx:
            copy.start()
        kz[0].send(0)
        yield
        with jax.named_scope("kx_wait"):
            for j in range(1, NX):
                kx[j - 1].wait_recv()
                kz[j].send(0)
        yield
        for s_at in range(4):
            for r in kz:
                r.wait(s_at)
                if s_at < 3:
                    r.send(s_at + 1)
                yield
        for copy in kx:
            copy.wait_send()
        yield

    def value_side():
        def v_rows(plane, planes, block, at, count):
            rows = pl.ds(pl.multiple_of(block * ROWS + at, 16), count)
            return vg.at[pl.ds(plane, planes), rows, :]

        vz = TwoStage(
            "vz", z, ROWS,
            lambda p, at, count: v_rows(p, 1, x, at, count),
            lambda p: device(p, x, y, c),
            (vz_s, vz_r),
        )
        vx = [
            Ring(
                "vx", NX, x,
                lambda p, i=i: v_rows(2 * i, 2, p, 0, ROWS),
                lambda p, h, i=i: v_rows(2 * i + h, 1, p, 0, ROWS),
                lambda p: device(z, p, y, c),
                [s.at[i] for s in vx_sem],
            )
            for i in range(4)
        ]
        drains.extend([vz, *vx])
        vz.start()
        yield
        vz.wait(0)
        vz.send(5)
        vz.send(4)
        vz.wait(1)
        vz.send(7)
        vz.send(6)
        yield
        vz.wait(2, 3, 4, 5, 6, 7)
        for r in vx:
            r.send(0)
        yield
        for r in vx:
            r.wait(0)
            r.send(1)
            if r is vx[1]:
                yield
        yield
        for r in vx:
            r.wait(1)
        yield

    def out_side():
        assert order_done.count("G") > 7 and order_done.count("V") > 5
        total, later = None, None
        for d in range(NZ):
            g = lax.rem(z + (NZ - d), NZ)
            part = dot(wts[d], vg[g])
            total = part if d == 0 else total + jnp.exp(later) * part
            later = cum[d] if d == 0 else later + cum[d]
        attended = total.astype(BF16)
        att[y, :, my_cols] = attended
        ring = TwoStage(
            "at", y, ROWS,
            lambda p, at, count: att.at[p, pl.ds(at, count), my_cols],
            lambda p: device(z, x, p, c),
            (at_s, at_r),
        )
        drains.append(ring)
        across = []

        def hand_over(i):
            p = lax.rem(y + NY + i, NY)
            ref = att.at[p, :, my_cols]
            copy = rdma(ref, ref, atp_s.at[i + 3], atp_r.at[i + 3], partner)
            copy.start()
            across.append(copy)

        ring.start()
        hand_over(0)
        yield
        ring.wait(0)
        ring.send(5)
        ring.send(4)
        ring.wait(1)
        ring.send(7)
        ring.send(6)
        hand_over(-2)
        hand_over(2)
        ring.wait(2, 3)
        hand_over(-1)
        hand_over(1)
        yield
        ring.wait(5, 7)
        hand_over(-3)
        hand_over(3)
        ring.wait(4, 6)
        hand_over(4)
        yield
        with jax.named_scope("at_pair_wait"):
            for copy in across:
                copy.wait_recv()
        l_wo.wait()
        total = dot(att[0], wo[pl.ds(0, 256), :])
        for i in range(1, NY):
            total += dot(att[i], wo[pl.ds(i * 256, 256), :])
        out_ab[0] = total.astype(BF16)
        for copy in across:
            copy.wait_send()
        yield

    back = {}

    def give_back(i, slots, value):
        first = slots[0] * CAP
        res[i, pl.ds(first, PART), :] = value.astype(BF16)
        if first == 0:
            ret[i, pl.ds(0, CAP), :] = value[0:CAP, :].astype(BF16)
        for slot in slots:
            if slot > 0:
                zz, xx = peer(slot, -1)
                at = pl.ds(slot * CAP, CAP)
                back[i, slot] = rdma(
                    res.at[i, at, :], ret.at[i, at, :], back_s.at[i, slot], back_r.at[i, slot],
                    device(zz, xx, y, c),
                )
                back[i, slot].start()

    def experts(part_at):
        base = part_at * PART
        yg = Ring(
            "yg", NY, y,
            lambda p: xg.at[p, pl.ds(base, PART), my_cols],
            None,
            lambda p: device(z, x, p, c),
            [s.at[part_at] for s in yg_sem],
        )
        drains.append(yg)
        across = {}

        def hand_over(i):
            p = lax.rem(y + (NY - i), NY)
            ref = xg.at[p, pl.ds(base, PART), my_cols]
            copy = rdma(ref, ref, ygp_s.at[part_at, i], ygp_r.at[part_at, i], partner)
            copy.start()
            across[i] = copy

        slots = range(base // CAP, (base + PART) // CAP)
        with jax.named_scope("a2a_wait"):
            for slot in slots:
                if slot > 0:
                    a2a[0, slot].wait_recv()
        yg.send(0)
        hand_over(0)
        yield
        if part_at == 0:
            for copy in l_gu:
                copy.wait()
            l_wd.wait()
        mine = pl.ds(base, PART)

        def multiply(i, start=False):
            with jax.named_scope("pair_wait"):
                across[i].wait_recv()
            p = lax.rem(y + (NY - i), NY)
            part = dot(xg[p, mine, :], wgu[pl.ds(pl.multiple_of(p * 256, 256), 256), :])
            if start:
                acc[mine, :] = part
            else:
                acc[mine, :] += part

        for s_at in range(3):
            yg.wait(s_at)
            if s_at < 2:
                yg.send(s_at + 1)
            hand_over(s_at + 1)
            hand_over(7 - s_at)
            if s_at == 1:
                with jax.named_scope("a2a_wait#far"):
                    for slot in slots:
                        if slot > 0:
                            a2a[1, slot].wait_recv()
                hand_over(4)
            if s_at == 0:
                multiply(0, True)
            else:
                multiply(s_at)
                multiply(8 - s_at)
            if s_at == 2:
                multiply(4)
            yield
        multiply(3)
        multiply(5)
        gate, up = acc[mine, 0:HD], acc[mine, HD : 2 * HD]
        hidden = (gate / (1.0 + jnp.exp(-gate)) * up).astype(BF16)
        with jax.named_scope("down"):
            part = dot(hidden, wd[...])
            for p in range(NY):
                lower = part[:, p * 256 : p * 256 + HD]
                upper = part[:, p * 256 + HD : (p + 1) * 256]
                po[p, mine, :] = jnp.where(c == 0, lower, upper)
                tosend[p, mine, :] = jnp.where(c == 0, upper, lower).astype(BF16)
        trade = rdma(
            tosend.at[:, mine, :], fromp.at[:, mine, :], ex_s.at[part_at], ex_r.at[part_at], partner
        )
        trade.start()
        yield
        right = device(z, x, lax.rem(y + 1, NY), c)
        left = device(z, x, lax.rem(y + NY - 1, NY), c)
        moved = []
        last = {}
        with jax.named_scope("trade_wait"):
            trade.wait_recv()
        value = po[opposite, mine, :] + fromp[opposite, mine, :].astype(F32)
        give_back(1, slots, value)
        for s_at in range(3):
            for way, i, sent, got, to, sems in (
                (0, 3 - s_at, sbr, rbr, right, (rs_sem[0], rs_sem[1])),
                (1, 5 + s_at, sbl, rbl, left, (rs_sem[2], rs_sem[3])),
            ):
                p = lax.rem(y + i, NY)
                value = po[p, mine, :] + fromp[p, mine, :].astype(F32)
                if s_at > 0:
                    with jax.named_scope(f"rs_wait#s={s_at}"):
                        last[way].wait_recv()
                    value = value + got[s_at - 1, mine, :].astype(F32)
                sent[s_at, mine, :] = value.astype(BF16)
                copy = rdma(
                    sent.at[s_at, mine, :], got.at[s_at, mine, :],
                    sems[0].at[part_at, s_at], sems[1].at[part_at, s_at], to,
                )
                copy.start()
                moved.append(copy)
                last[way] = copy
            yield
        with jax.named_scope("rs_wait#s=4"):
            last[0].wait_recv()
            last[1].wait_recv()
        value = po[y, mine, :] + fromp[y, mine, :].astype(F32)
        value = value + rbr[2, mine, :].astype(F32) + rbl[2, mine, :].astype(F32)
        give_back(0, slots, value)
        yield
        for copy in (*across.values(), trade, *moved):
            copy.wait_send()
        yield

    def route_weights():
        l_rw.wait()
        weight = first * rw[0:1, :] + second * rw[1:2, :]
        w_high = weight.astype(BF16)
        w_low = (weight - w_high.astype(F32)).astype(BF16)
        mask = pt[...].astype(F32)
        wth[...] = (dot(spread, w_high) * mask).T.astype(BF16)
        wtl[...] = (dot(spread, w_low) * mask).T.astype(BF16)
        yield

    def combined(i):
        with jax.named_scope(f"back_wait#i={i}"):
            for slot in range(1, NEP):
                back[i, slot].wait_recv()
        return dot(wth[...], ret[i]) + dot(wtl[...], ret[i])

    half = ROWS // 2
    hops = []

    def opposite_part():
        assert "W" in order_done
        part = combined(1).astype(BF16)
        far[0] = part[:half, :]
        far[1] = part[half:, :]
        between = [device(z, x, lax.rem(y + a, NY), c) for a in (2, NY - 2)]
        for i in range(2):
            hops.append(rdma(far.at[i], far.at[i + 2], far_s.at[i], far_r.at[i], between[i]))
            hops[i].start()
        yield
        for i in range(2):
            with jax.named_scope("far_wait"):
                hops[i].wait_recv()
            hops.append(
                rdma(far.at[i + 2], farin.at[i], far_s.at[i + 2], far_r.at[i + 2], between[i])
            )
            hops[i + 2].start()
        yield

    def combine():
        with jax.named_scope("farin_wait"):
            hops[2].wait_recv()
            hops[3].wait_recv()
        sums = combined(0)
        for i in range(2):
            rows = slice(i * half, (i + 1) * half)
            out_ab[1, rows, :] = (sums[rows, :] + farin[i].astype(F32)).astype(BF16)
        yield

    def drain():
        for copy in (*a2a.values(), *hops):
            copy.wait_send()
        for slot in range(1, NEP):
            back[1, slot].wait_send()
        for ring in drains:
            ring.drain()
        yield

    tasks = {str(i): experts(i) for i in range(PARTS)}
    tasks.update({"K": key_side(), "V": value_side(), "O": out_side(), "D": opposite_rows(), "W": route_weights(), "C": combine(), "G": groups(), "F": opposite_part(), "X": drain()})
    for name in ORDER:
        order_done.append(name)
        if name in tasks:
            try:
                with jax.named_scope(name):
                    next(tasks[name])
            except StopIteration:
                del tasks[name]
    for rest in tasks.values():
        with jax.named_scope("rest"):
            for _ in rest:
                pass
    with jax.named_scope("drain"):
        for slot in range(1, NEP):
            back[0, slot].wait_send()


def ring_sems(count, steps):
    return [pltpu.SemaphoreType.DMA((count, steps))] * 4


def on_device(
    mixer_input, mixer_gain, query_weight, key_weight, value_weight, score_offset, out_weight,
    expert_input, expert_gain, route_ids, route_weights, gate_weight, up_weight, down_weight,
):
    hbm = pl.BlockSpec(memory_space=pl.ANY)
    vmem = pl.BlockSpec(memory_space=pltpu.VMEM)
    dma = pltpu.SemaphoreType.DMA
    out = pltpu.VMEM((2, ROWS, HD), BF16)
    scratch = [
        pltpu.VMEM((1, 1), F32),
        pltpu.VMEM((ROWS, D), BF16),
        pltpu.VMEM((1, D), F32),
        pltpu.VMEM((D, 3 * HD), BF16),
        pltpu.VMEM((D, HD), BF16),
        pltpu.VMEM((ROWS, D), BF16),
        pltpu.VMEM((1, D), F32),
        pltpu.VMEM((2, ROWS), jnp.int32),
        pltpu.VMEM((2, ROWS), F32),
        pltpu.VMEM((D, 2 * HD), BF16),
        pltpu.VMEM((HD, D), BF16),
        pltpu.VMEM((ROWS, D), BF16),
        pltpu.VMEM((ROWS, HD), BF16),
        pltpu.VMEM((NEP * ROWS, HD), BF16),
        pltpu.VMEM((NZ, NX * ROWS, HD), BF16),
        pltpu.VMEM((NZ, ROWS, NX * ROWS), BF16),
        pltpu.VMEM((NZ, ROWS, ROWS), F32),
        pltpu.VMEM((256, 256), BF16),
        pltpu.VMEM((NY, ROWS, 2 * HD), BF16),
        pltpu.VMEM((2, SLOTS, HD), BF16),
        pltpu.VMEM((SLOTS, ROWS), BF16),
        pltpu.VMEM((ROWS, SLOTS), BF16),
        pltpu.VMEM((ROWS, SLOTS), BF16),
        pltpu.VMEM((NY, SLOTS, 2 * HD), BF16),
        pltpu.VMEM((SLOTS, 2 * HD), F32),
        pltpu.VMEM((NY, SLOTS, HD), F32),
        pltpu.VMEM((NY, SLOTS, HD), BF16),
        pltpu.VMEM((NY, SLOTS, HD), BF16),
        pltpu.VMEM((3, SLOTS, HD), BF16),
        pltpu.VMEM((3, SLOTS, HD), BF16),
        pltpu.VMEM((3, SLOTS, HD), BF16),
        pltpu.VMEM((3, SLOTS, HD), BF16),
        pltpu.VMEM((2, SLOTS, HD), BF16),
        pltpu.VMEM((2, SLOTS, HD), BF16),
        pltpu.VMEM((4, ROWS // 2, HD), BF16),
        pltpu.VMEM((2, ROWS // 2, HD), BF16),
    ]
    semaphores = [
        dma((14,)),
        dma((2, NEP)), dma((2, NEP)), dma((2, NEP)), dma((2, NEP)), dma((4,)), dma((4,)),
        dma((NX,)), dma((NX,)), ring_sems(4, 4), dma((8,)), dma((8,)), ring_sems(4, 2),
        dma((8,)), dma((8,)), dma((NY,)), dma((NY,)),
        ring_sems(PARTS, 3), dma((PARTS, NY)), dma((PARTS, NY)),
        dma((PARTS,)), dma((PARTS,)), ring_sems(PARTS, 3),
    ]
    flat, tree = jax.tree.flatten(semaphores)

    def body(*refs):
        def scoped(*sems):
            mega(*refs, *jax.tree.unflatten(tree, sems))

        pl.run_scoped(scoped, *flat)

    both = pl.pallas_call(
        body,
        out_shape=out,
        in_specs=[hbm] * 14,
        out_specs=vmem,
        scratch_shapes=scratch,
        compiler_params=pltpu.CompilerParams(
            collective_id=0, has_side_effects=True, vmem_limit_bytes=60 * 1024 * 1024
        ),
        name="both_halves",
    )(
        score_offset.reshape(1, 1),
        mixer_input, mixer_gain.reshape(1, D), query_weight, key_weight, value_weight, out_weight,
        expert_input, expert_gain.reshape(1, D), route_ids.T, route_weights.T,
        gate_weight.reshape(D, HD), up_weight.reshape(D, HD), down_weight.reshape(HD, D),
    )
    return both[0], both[1]


def solution(mesh):
    in_specs = (
        P("ep", None),
        P(),
        P(None, "tp"),
        P(None, "tp"),
        P(None, "tp"),
        P("tp"),
        P(None, "tp"),
        P("ep", None),
        P(),
        P("ep", None),
        P("ep", None),
        P("ep", None, "tp"),
        P("ep", None, "tp"),
        P("ep", "tp", None),
    )
    out_specs = (P("ep", "tp"), P("ep", "tp"))
    return jax.shard_map(
        on_device, mesh=mesh, in_specs=in_specs, out_specs=out_specs, check_vma=False
    )
```
